32 devices in a mesh: sp: 16 (over z, y, x), tp: 2 (over core).
Axes of the slice: x: 2, y: 2, z: 4, core: 2. Of those that a mesh axis runs over, the one named last changes fastest.
Arguments:
- residual_in: bfloat16 [4096, 2048], P('sp'), may hold values from -6 to 6
- mixer_input: bfloat16 [2048, 4096], P('tp', 'sp'), may hold values from -6 to 6
- branch_gate: bfloat16 [2048, 4096], P('tp', 'sp'), may hold values from -6 to 6
- conv_taps: bfloat16 [2048, 4], P('tp'), may hold values from -3 to 3
- recur_weight: bfloat16 [32, 64, 64], P('tp'), may hold values from -0.75 to 0.75
- admit_weight: bfloat16 [32, 64, 64], P('tp'), may hold values from -0.75 to 0.75
- decay_param: float32 [2048], P('tp'), may hold values from 4 to 16
- decay_extra: float32 [2048, 4096], P('tp', 'sp'), may hold values from -1 to 0
- out_weight: bfloat16 [2048, 2048], P('tp'), may hold values from -0.375 to 0.375
- norm_gain: bfloat16 [2048], replicated, may hold values from 0.099609375 to 1.8984375
- gate_weight: bfloat16 [2048, 5632], P('sp', 'tp'), may hold values from -0.125 to 0.125
- up_weight: bfloat16 [2048, 5632], P('sp', 'tp'), may hold values from -0.125 to 0.125
- down_weight: bfloat16 [2048, 5632], P('sp', 'tp'), may hold values from -0.15625 to 0.15625
Outputs:
- layer_out: bfloat16 [4096, 2048], P('sp')
The draws below stay inside these ranges and needn't reach their ends.
All inputs are finite; a program needn't handle non-finite values.
Results may differ from the reference program's by a relative error of at most 0.019.
Values may be sent and summed in bfloat16 or wider, within the bound.
A program may use at most 128 MiB of HBM per device.

```python
import jax
import jax.numpy as jnp
from jax import lax

D = 2048
W = 2048
BLOCKS = 32
BLOCK = 64
FF = 5632
KERNEL = 4
TOK_DEV = 256
TOKENS = 4096
N_SP = 16
N_TP = 2


def draw_decay_param(key, part):
    pick_key, slow_key, fast_key = jax.random.split(key, 3)
    slow_share = 0.5
    slow_rate = jax.random.uniform(slow_key, (W,), jnp.float32, 0.2, 0.6) / (4.0 * TOKENS)
    fast_rate = jnp.exp(jax.random.uniform(fast_key, (W,), jnp.float32, jnp.log(0.0025), jnp.log(0.01)))
    chosen = jax.random.uniform(pick_key, (W,), jnp.float32) < slow_share
    picked_rate = jnp.where(chosen, slow_rate, fast_rate)
    return (-jnp.log(jnp.expm1(picked_rate))).astype(jnp.float32)


def draw_decay_extra(key, part):
    level_key, spot_key, loss_key = jax.random.split(key, 3)
    low_end = 0.15
    high_end = 0.9
    block_count = TOKENS // TOK_DEV
    levels = jnp.exp(jax.random.uniform(level_key, (W, block_count), jnp.float32, jnp.log(low_end), jnp.log(high_end))) / TOKENS
    steady = -jnp.repeat(levels, TOK_DEV, axis=1)
    spots = jax.random.randint(spot_key, (3,), 0, TOKENS)
    losses = jnp.log1p(-jax.random.uniform(loss_key, (W, 3), jnp.float32, 0.2, 0.4))
    positions = jnp.arange(TOKENS)
    result_field = steady
    for which in range(3):
        hit_row = (positions == spots[which]).astype(jnp.float32)
        result_field = result_field + losses[:, which:which + 1] * hit_row[None, :]
    return result_field.astype(jnp.float32)


def shard_levels(key, shape, cuts, smallest, largest):
    loudness = 1.0
    for position, shards_of in cuts:
        steps = jax.random.uniform(jax.random.fold_in(jax.random.fold_in(key, 6), position), (shards_of,), jnp.float32, smallest / len(cuts), largest / len(cuts))
        loudness = loudness * jnp.repeat(jnp.exp(steps), shape[position] // shards_of).reshape((-1,) + (1,) * (len(shape) - 1 - position))
    return loudness


def normal_values(stream_key, shape, deviation, most, pieces=(), held_as=jnp.bfloat16):
    factor_of = shard_levels(stream_key, shape, pieces, -0.22, 0.18) if pieces else 1.0
    drawn = jax.random.normal(stream_key, shape, jnp.float32) * deviation * factor_of
    return jnp.minimum(jnp.maximum(drawn, -most), most).astype(held_as)


def setup_inputs(seed: int = 0) -> dict:
    keys = jax.random.split(jax.random.key(seed), 14)
    return {
        "residual_in": normal_values(keys[0], (TOKENS, D), 1.0, 6.0, ((0, 16),)),
        "mixer_input": normal_values(keys[1], (W, TOKENS), 1.0, 6.0, ((0, 2), (1, 16))),
        "branch_gate": normal_values(keys[2], (W, TOKENS), 1.0, 6.0, ((0, 2), (1, 16))),
        "conv_taps": normal_values(keys[3], (W, KERNEL), KERNEL ** -0.5, 3.0, ((0, 2),)),
        "recur_weight": normal_values(keys[4], (BLOCKS, BLOCK, BLOCK), BLOCK ** -0.5, 0.75, ((0, 2),)),
        "admit_weight": normal_values(keys[5], (BLOCKS, BLOCK, BLOCK), BLOCK ** -0.5, 0.75, ((0, 2),)),
        "decay_param": draw_decay_param(jax.random.fold_in(keys[13], 71), 0),
        "decay_extra": draw_decay_extra(jax.random.fold_in(keys[13], 71), 0),
        "out_weight": normal_values(keys[8], (W, D), (W // 8) ** -0.5, 0.375, ((0, 2),)),
        "norm_gain": jnp.clip(1.0 + 0.18 * jax.random.normal(keys[9], (D,), jnp.float32), 0.099609375, 1.8984375).astype(jnp.bfloat16),
        "gate_weight": normal_values(keys[10], (D, FF), D ** -0.5, 0.125, ((0, 16), (1, 2))),
        "up_weight": normal_values(keys[11], (D, FF), D ** -0.5, 0.125, ((0, 16), (1, 2))),
        "down_weight": normal_values(keys[12], (D, FF), (FF // 4) ** -0.5, 0.15625, ((0, 16), (1, 2))),
    }


def block_gates(weight, signal):
    groups = weight.shape[0]
    grouped = signal.astype(jnp.float32).reshape(groups, weight.shape[1], signal.shape[1])
    mapped = jnp.einsum('gij,git->gjt', weight.astype(jnp.float32), grouped)
    return jax.nn.sigmoid(mapped.reshape(signal.shape))

def link_pairs(earlier, latter):
    return (earlier[0] * latter[0], latter[0] * earlier[1] + latter[1])

def reference(residual_in, mixer_input, branch_gate, conv_taps, recur_weight, admit_weight, decay_param, decay_extra, out_weight, norm_gain, gate_weight, up_weight, down_weight):
    tap_count = conv_taps.shape[1]
    length = mixer_input.shape[1]
    padded = jnp.pad(mixer_input.astype(jnp.float32), ((0, 0), (tap_count - 1, 0)))
    tap_values = conv_taps.astype(jnp.float32)
    conv_sum = jnp.zeros(mixer_input.shape, jnp.float32)
    for tap in range(tap_count):
        conv_sum = conv_sum + tap_values[:, tap:tap + 1] * padded[:, tap:tap + length]
    conv_out = conv_sum.astype(jnp.bfloat16)
    recur_gate = block_gates(recur_weight, conv_out)
    admit_gate = block_gates(admit_weight, conv_out)
    base_rate = jax.nn.softplus(-decay_param.astype(jnp.float32))[:, None]
    log_decay = -8.0 * recur_gate * base_rate + decay_extra
    decay_step = jnp.exp(log_decay)
    drive_term = jnp.sqrt(-jnp.expm1(2.0 * log_decay)) * admit_gate * conv_out.astype(jnp.float32)
    running, states = lax.associative_scan(link_pairs, (decay_step, drive_term), axis=1)
    gate_act = jax.nn.gelu(branch_gate.astype(jnp.float32), approximate=True)
    mixed_out = (states * gate_act).astype(jnp.bfloat16)
    model_width = residual_in.shape[1]
    split_width = gate_weight.shape[1] // N_TP
    res_blocks = residual_in.reshape(N_SP, TOK_DEV, model_width)
    mix_blocks = mixed_out.reshape(mixed_out.shape[0], N_SP, TOK_DEV).transpose(1, 0, 2)
    gain_wide = norm_gain.astype(jnp.float32)
    down_split = down_weight.astype(jnp.float32).reshape(model_width, N_TP, split_width)

    def one_block(pair):
        resid, mix_block = pair
        branch = jnp.dot(mix_block.T, out_weight, preferred_element_type=jnp.float32)
        middle = (resid.astype(jnp.float32) + branch).astype(jnp.bfloat16)
        middle_wide = middle.astype(jnp.float32)
        row_scale = lax.rsqrt(lax.optimization_barrier(jnp.mean(middle_wide * middle_wide, axis=1, keepdims=True)) + 1e-06)
        normed = (middle_wide * row_scale * gain_wide).astype(jnp.bfloat16)
        gate_pre = jnp.dot(normed, gate_weight, preferred_element_type=jnp.float32)
        up_pre = jnp.dot(normed, up_weight, preferred_element_type=jnp.float32)
        hidden = (jax.nn.silu(gate_pre) * up_pre).astype(jnp.bfloat16)
        hidden_split = hidden.astype(jnp.float32).reshape(hidden.shape[0], N_TP, split_width)
        partial_value = jnp.einsum('tkf,dkf->ktd', hidden_split, down_split).astype(jnp.bfloat16)
        partial_value = lax.optimization_barrier(partial_value)
        channel_out = lax.optimization_barrier(jnp.sum(partial_value.astype(jnp.float32), axis=0))
        return (middle.astype(jnp.float32) + channel_out).astype(jnp.bfloat16)
    layer_blocks = lax.map(one_block, (res_blocks, mix_blocks))
    return layer_blocks.reshape(N_SP * TOK_DEV, model_width)
```

```python
import functools

import jax
import jax.numpy as jnp
from jax import lax
from jax.experimental import pallas as pl
from jax.experimental.pallas import tpu as pltpu
from jax.sharding import PartitionSpec as P

MESH = pl.DeviceIdType.MESH
LANES = 128


def neg_expm1(v):
    series = jnp.full_like(v, 1.0)
    for k in range(9, 1, -1):
        series = 1.0 + series * v * (1.0 / k)
    return jnp.where(v > -0.5, -v * series, 1.0 - jnp.exp(v))


def mixer_kernel(
    n,
    x_ref,
    halo_ref,
    bg_ref,
    extra_ref,
    taps_ref,
    rate_ref,
    wr_ref,
    wa_ref,
    out_ref,
    state_s,
    run_s,
    ends_s,
    all_s,
    in_s,
    send_sem,
    recv_sem,
):
    me = lax.axis_index("sp")
    barrier = pltpu.get_barrier_semaphore()

    def greet(k, carry):
        pl.semaphore_signal(
            barrier, inc=1, device_id={"sp": lax.rem(me + k, n)}, device_id_type=MESH
        )
        return carry

    lax.fori_loop(1, n, greet, 0)
    channels, length = x_ref.shape
    block = wr_ref.shape[1]
    groups = channels // LANES
    tap_count = taps_ref.shape[1]
    lane = lax.broadcasted_iota(jnp.int32, (LANES, length), 1)

    def local(g, carry):
        rows = pl.ds(pl.multiple_of(g * LANES, LANES), LANES)
        wide = jnp.concatenate(
            [halo_ref[rows, :].astype(jnp.float32), x_ref[rows, :].astype(jnp.float32)], axis=1
        )
        taps = taps_ref[rows, :]
        total = taps[:, tap_count - 1 :] * wide[:, LANES:]
        for tap in range(tap_count - 2, -1, -1):
            total = total + taps[:, tap : tap + 1] * pltpu.roll(wide, tap_count - 1 - tap, 1)[:, LANES:]
        conv = total.astype(jnp.bfloat16)
        per = LANES // block
        recur, admit = [], []
        for b in range(per):
            part = conv[b * block : (b + 1) * block]
            recur.append(jnp.dot(wr_ref[g * per + b], part, preferred_element_type=jnp.float32))
            admit.append(jnp.dot(wa_ref[g * per + b], part, preferred_element_type=jnp.float32))
        recur = jax.nn.sigmoid(jnp.concatenate(recur, axis=0))
        admit = jax.nn.sigmoid(jnp.concatenate(admit, axis=0))
        log_decay = recur * rate_ref[rows, :] + extra_ref[rows, :]
        a = jnp.exp(log_decay)
        b = jnp.sqrt(neg_expm1(2.0 * log_decay)) * admit * conv.astype(jnp.float32)
        shift = 1
        while shift < length:
            seen = lane >= shift
            b = b + a * jnp.where(seen, pltpu.roll(b, shift, 1), 0.0)
            a = a * jnp.where(seen, pltpu.roll(a, shift, 1), 1.0)
            shift *= 2
        state_s[rows, :] = b
        run_s[rows, :] = a
        ends_s[pl.ds(g, 1), :] = a[:, length - LANES :].T[LANES - 1 :]
        ends_s[pl.ds(groups + g, 1), :] = b[:, length - LANES :].T[LANES - 1 :]
        return carry

    lax.fori_loop(0, groups, local, 0)
    pl.semaphore_wait(barrier, n - 1)

    def copy_to(k):
        return pltpu.make_async_remote_copy(
            src_ref=ends_s,
            dst_ref=all_s.at[k - 1],
            send_sem=send_sem.at[k - 1],
            recv_sem=recv_sem.at[k - 1],
            device_id={"sp": lax.rem(me + k, n)},
            device_id_type=MESH,
        )

    def send(k, carry):
        copy_to(k).start()
        return carry

    lax.fori_loop(1, n, send, 0)

    def finish(k, carry):
        copy_to(k).wait()
        return carry

    lax.fori_loop(1, n, finish, 0)

    def fold(i, before):
        k = n - 1 - i
        part = all_s[k - 1]
        new = part[:groups] * before + part[groups:]
        return jnp.where(k <= me, new, before)

    in_s[...] = lax.fori_loop(0, n - 1, fold, jnp.zeros((groups, LANES), jnp.float32))

    def close(g, carry):
        rows = pl.ds(pl.multiple_of(g * LANES, LANES), LANES)
        entering = jnp.broadcast_to(in_s[pl.ds(g, 1), :], (LANES, LANES)).T
        entering = jnp.concatenate([entering] * (length // LANES), axis=1)
        states = state_s[rows, :] + run_s[rows, :] * entering
        v = bg_ref[rows, :].astype(jnp.float32)
        act = 0.5 * v * (1.0 + jnp.tanh(0.7978845608028654 * (v + 0.044715 * v * v * v)))
        out_ref[rows, :] = (states * act).astype(jnp.bfloat16)
        return carry

    lax.fori_loop(0, groups, close, 0)


def mixer(n, x, halo, bg, extra, taps, rate, wr, wa):
    channels, length = x.shape
    groups = channels // LANES
    vmem = pl.BlockSpec(memory_space=pltpu.VMEM)
    return pl.pallas_call(
        functools.partial(mixer_kernel, n),
        out_shape=jax.ShapeDtypeStruct((channels, length), jnp.bfloat16),
        in_specs=[vmem] * 8,
        out_specs=vmem,
        scratch_shapes=[
            pltpu.VMEM((channels, length), jnp.float32),
            pltpu.VMEM((channels, length), jnp.float32),
            pltpu.VMEM((2 * groups, LANES), jnp.float32),
            pltpu.VMEM((n - 1, 2 * groups, LANES), jnp.float32),
            pltpu.VMEM((groups, LANES), jnp.float32),
            pltpu.SemaphoreType.DMA((n - 1,)),
            pltpu.SemaphoreType.DMA((n - 1,)),
        ],
        compiler_params=pltpu.CompilerParams(
            collective_id=0, has_side_effects=True, vmem_limit_bytes=24 << 20
        ),
        cost_estimate=pl.CostEstimate(
            flops=200 * channels * length, bytes_accessed=12 * channels * length, transcendentals=0
        ),
        name="mixer",
    )(x, halo, bg, extra, taps, rate, wr, wa)


def on_device(
    residual_in,
    mixer_input,
    branch_gate,
    conv_taps,
    recur_weight,
    admit_weight,
    decay_param,
    decay_extra,
    out_weight,
    norm_gain,
    gate_weight,
    up_weight,
    down_weight,
):
    n = lax.axis_size("sp")
    length = mixer_input.shape[1]
    halo = lax.ppermute(
        mixer_input[:, length - LANES :], "sp", [(i, i + 1) for i in range(n - 1)]
    )
    rate = -8.0 * jax.nn.softplus(-decay_param)[:, None]
    mixed_out = mixer(
        n,
        mixer_input,
        halo,
        branch_gate,
        decay_extra,
        conv_taps.astype(jnp.float32),
        rate,
        recur_weight.transpose(0, 2, 1),
        admit_weight.transpose(0, 2, 1),
    )
    row_count = residual_in.shape[0]
    partial_value = lax.dot_general(
        mixed_out, out_weight, (((0,), (0,)), ((), ())), preferred_element_type=jnp.float32
    )
    branch = lax.psum(partial_value.astype(jnp.bfloat16), "tp").astype(jnp.float32)
    middle = (residual_in.astype(jnp.float32) + branch).astype(jnp.bfloat16)
    middle_wide = middle.astype(jnp.float32)
    row_scale = lax.rsqrt(jnp.mean(middle_wide * middle_wide, axis=1, keepdims=True) + 1e-06)
    normed = (middle_wide * row_scale * norm_gain.astype(jnp.float32)).astype(jnp.bfloat16)
    gate_pre = jnp.dot(
        normed,
        lax.all_gather(gate_weight, "sp", axis=0, tiled=True),
        preferred_element_type=jnp.float32,
    )
    up_pre = jnp.dot(
        normed,
        lax.all_gather(up_weight, "sp", axis=0, tiled=True),
        preferred_element_type=jnp.float32,
    )
    down_whole = lax.all_gather(down_weight, "sp", axis=0, tiled=True)
    hidden = (jax.nn.silu(gate_pre) * up_pre).astype(jnp.bfloat16)
    share = row_count // lax.axis_size("tp")
    channel_out = lax.psum_scatter(
        lax.dot_general(
            hidden, down_whole, (((1,), (1,)), ((), ())), preferred_element_type=jnp.float32
        ).astype(jnp.bfloat16),
        "tp",
        scatter_dimension=0,
        tiled=True,
    ).astype(jnp.float32)
    first_row = lax.axis_index("tp") * share
    own_rows = lax.dynamic_slice_in_dim(middle, first_row, share, 0)
    layer_rows = (own_rows.astype(jnp.float32) + channel_out).astype(jnp.bfloat16)
    return lax.all_gather(layer_rows, "tp", axis=0, tiled=True)


def solution(mesh):
    placed = (
        P("sp", None),
        P("tp", "sp"),
        P("tp", "sp"),
        P("tp", None),
        P("tp", None, None),
        P("tp", None, None),
        P("tp"),
        P("tp", "sp"),
        P("tp", None),
        P(),
        P("sp", "tp"),
        P("sp", "tp"),
        P("sp", "tp"),
    )
    return jax.shard_map(
        on_device, mesh=mesh, in_specs=placed, out_specs=P("sp", None), check_vma=False
    )
```

```python
import functools

import jax
import jax.numpy as jnp
from jax import lax
from jax.experimental import pallas as pl
from jax.experimental.pallas import tpu as pltpu
from jax.sharding import PartitionSpec as P

MESH = pl.DeviceIdType.MESH
LANES = 128


def neg_expm1(v):
    series = jnp.full_like(v, 1.0)
    for k in range(9, 1, -1):
        series = 1.0 + series * v * (1.0 / k)
    return jnp.where(v > -0.5, -v * series, 1.0 - jnp.exp(v))


def mixer_kernel(
    n,
    x_ref,
    halo_ref,
    bg_ref,
    extra_ref,
    taps_ref,
    rate_ref,
    wr_ref,
    wa_ref,
    out_ref,
    state_s,
    run_s,
    ends_s,
    all_s,
    in_s,
    send_sem,
    recv_sem,
):
    me = lax.axis_index("sp")
    barrier = pltpu.get_barrier_semaphore()

    def greet(k, carry):
        pl.semaphore_signal(
            barrier, inc=1, device_id={"sp": lax.rem(me + k, n)}, device_id_type=MESH
        )
        return carry

    lax.fori_loop(1, n, greet, 0)
    channels, length = x_ref.shape
    block = wr_ref.shape[1]
    groups = channels // LANES
    tap_count = taps_ref.shape[1]
    lane = lax.broadcasted_iota(jnp.int32, (LANES, length), 1)

    def local(g, carry):
        rows = pl.ds(pl.multiple_of(g * LANES, LANES), LANES)
        wide = jnp.concatenate(
            [halo_ref[rows, :].astype(jnp.float32), x_ref[rows, :].astype(jnp.float32)], axis=1
        )
        taps = taps_ref[rows, :]
        total = taps[:, tap_count - 1 :] * wide[:, LANES:]
        for tap in range(tap_count - 2, -1, -1):
            total = total + taps[:, tap : tap + 1] * pltpu.roll(wide, tap_count - 1 - tap, 1)[:, LANES:]
        conv = total.astype(jnp.bfloat16)
        per = LANES // block
        recur, admit = [], []
        for b in range(per):
            part = conv[b * block : (b + 1) * block]
            recur.append(jnp.dot(wr_ref[g * per + b], part, preferred_element_type=jnp.float32))
            admit.append(jnp.dot(wa_ref[g * per + b], part, preferred_element_type=jnp.float32))
        recur = jax.nn.sigmoid(jnp.concatenate(recur, axis=0))
        admit = jax.nn.sigmoid(jnp.concatenate(admit, axis=0))
        log_decay = recur * rate_ref[rows, :] + extra_ref[rows, :]
        a = jnp.exp(log_decay)
        b = jnp.sqrt(neg_expm1(2.0 * log_decay)) * admit * conv.astype(jnp.float32)
        shift = 1
        while shift < length:
            seen = lane >= shift
            b = b + a * jnp.where(seen, pltpu.roll(b, shift, 1), 0.0)
            a = a * jnp.where(seen, pltpu.roll(a, shift, 1), 1.0)
            shift *= 2
        state_s[rows, :] = b
        run_s[rows, :] = a
        ends_s[pl.ds(g, 1), :] = a[:, length - LANES :].T[LANES - 1 :]
        ends_s[pl.ds(groups + g, 1), :] = b[:, length - LANES :].T[LANES - 1 :]
        return carry

    lax.fori_loop(0, groups, local, 0)
    pl.semaphore_wait(barrier, n - 1)

    def copy_to(k):
        return pltpu.make_async_remote_copy(
            src_ref=ends_s,
            dst_ref=all_s.at[k - 1],
            send_sem=send_sem.at[k - 1],
            recv_sem=recv_sem.at[k - 1],
            device_id={"sp": lax.rem(me + k, n)},
            device_id_type=MESH,
        )

    def send(k, carry):
        copy_to(k).start()
        return carry

    lax.fori_loop(1, n, send, 0)

    def finish(k, carry):
        copy_to(k).wait()
        return carry

    lax.fori_loop(1, n, finish, 0)

    def fold(i, before):
        k = n - 1 - i
        part = all_s[k - 1]
        new = part[:groups] * before + part[groups:]
        return jnp.where(k <= me, new, before)

    in_s[...] = lax.fori_loop(0, n - 1, fold, jnp.zeros((groups, LANES), jnp.float32))

    def close(g, carry):
        rows = pl.ds(pl.multiple_of(g * LANES, LANES), LANES)
        entering = jnp.broadcast_to(in_s[pl.ds(g, 1), :], (LANES, LANES)).T
        entering = jnp.concatenate([entering] * (length // LANES), axis=1)
        states = state_s[rows, :] + run_s[rows, :] * entering
        v = bg_ref[rows, :].astype(jnp.float32)
        act = 0.5 * v * (1.0 + jnp.tanh(0.7978845608028654 * (v + 0.044715 * v * v * v)))
        out_ref[rows, :] = (states * act).astype(jnp.bfloat16)
        return carry

    lax.fori_loop(0, groups, close, 0)


def mixer(n, x, halo, bg, extra, taps, rate, wr, wa):
    channels, length = x.shape
    groups = channels // LANES
    vmem = pl.BlockSpec(memory_space=pltpu.VMEM)
    return pl.pallas_call(
        functools.partial(mixer_kernel, n),
        out_shape=jax.ShapeDtypeStruct((channels, length), jnp.bfloat16),
        in_specs=[vmem] * 8,
        out_specs=vmem,
        scratch_shapes=[
            pltpu.VMEM((channels, length), jnp.float32),
            pltpu.VMEM((channels, length), jnp.float32),
            pltpu.VMEM((2 * groups, LANES), jnp.float32),
            pltpu.VMEM((n - 1, 2 * groups, LANES), jnp.float32),
            pltpu.VMEM((groups, LANES), jnp.float32),
            pltpu.SemaphoreType.DMA((n - 1,)),
            pltpu.SemaphoreType.DMA((n - 1,)),
        ],
        compiler_params=pltpu.CompilerParams(
            collective_id=0, has_side_effects=True, vmem_limit_bytes=24 << 20
        ),
        cost_estimate=pl.CostEstimate(
            flops=200 * channels * length, bytes_accessed=12 * channels * length, transcendentals=0
        ),
        name="mixer",
    )(x, halo, bg, extra, taps, rate, wr, wa)


def layer_kernel(
    n,
    split,
    x_ref,
    halo_ref,
    bg_ref,
    extra_ref,
    taps_ref,
    rate_ref,
    wr_ref,
    wa_ref,
    ow_ref,
    res_ref,
    gain_ref,
    packed_ref,
    wide_ref,
    tok_ref,
    mid_ref,
    state_s,
    run_s,
    ends_s,
    all_s,
    in_s,
    mix_s,
    part_s,
    part_r,
    nrm_s,
    own_s,
    send_sem,
    recv_sem,
    zs_sem,
    zr_sem,
    ps_sem,
    pr_sem,
    fs_sem,
    fr_sem,
    ts_sem,
    tr_sem,
    bs_sem,
    br_sem,
    cs_sem,
    cr_sem,
    own_sem,
):
    me = lax.axis_index("sp")
    core = lax.axis_index("tp")
    plane = n // split
    rank, spot = me // plane, lax.rem(me, plane)
    barrier = pltpu.get_barrier_semaphore()

    def greet(k, carry):
        pl.semaphore_signal(
            barrier, inc=1, device_id={"sp": lax.rem(me + k, n)}, device_id_type=MESH
        )
        return carry

    lax.fori_loop(1, n, greet, 0)
    pl.semaphore_signal(barrier, inc=1, device_id={"tp": 1 - core}, device_id_type=MESH)
    pl.semaphore_wait(barrier, n)

    depth = packed_ref.shape[3]
    span = packed_ref.shape[2]
    kinds = packed_ref.shape[1]

    def columns(source):
        return pl.ds(pl.multiple_of(source * depth, depth), depth)

    def remote(src, dst, ssem, rsem, where):
        return pltpu.make_async_remote_copy(
            src_ref=src, dst_ref=dst, send_sem=ssem, recv_sem=rsem,
            device_id=where, device_id_type=MESH,
        )

    def z_copy(c, k):
        to = lax.rem(rank + k, split)
        return remote(
            packed_ref.at[to, c], wide_ref.at[c, :, columns(me)],
            zs_sem.at[c, k - 1], zr_sem.at[c, k - 1], {"sp": to * plane + spot},
        )

    def z_landed(c, k):
        source = lax.rem(rank - k + split, split) * plane + spot
        return remote(
            packed_ref.at[rank, c], wide_ref.at[c, :, columns(source)],
            zs_sem.at[c, k - 1], zr_sem.at[c, k - 1], {"sp": source},
        )

    def own_copy(c, m):
        return remote(
            packed_ref.at[rank, c], wide_ref.at[c, :, columns(me)],
            ps_sem.at[c, m - 1], pr_sem.at[c, m - 1],
            {"sp": rank * plane + lax.rem(spot + m, plane)},
        )

    def own_landed(c, m):
        source = rank * plane + lax.rem(spot - m + plane, plane)
        return remote(
            packed_ref.at[rank, c], wide_ref.at[c, :, columns(source)],
            ps_sem.at[c, m - 1], pr_sem.at[c, m - 1], {"sp": source},
        )

    def pass_copy(c, k, m):
        source = lax.rem(rank - k + split, split) * plane + spot
        window = wide_ref.at[c, :, columns(source)]
        return remote(
            window, window, fs_sem.at[c, k - 1, m - 1], fr_sem.at[c, k - 1, m - 1],
            {"sp": rank * plane + lax.rem(spot + m, plane)},
        )

    def pass_landed(c, k, m):
        behind = lax.rem(spot - m + plane, plane)
        source = lax.rem(rank - k + split, split) * plane + behind
        window = wide_ref.at[c, :, columns(source)]
        return remote(
            window, window, fs_sem.at[c, k - 1, m - 1], fr_sem.at[c, k - 1, m - 1],
            {"sp": rank * plane + behind},
        )

    def z_start(c):
        for k in range(1, split):
            z_copy(c, k).start()

    def z_pass(c):
        for k in range(1, split):
            z_landed(c, k).wait_recv()
            for m in range(1, plane):
                pass_copy(c, k, m).start()

    z_start(0)
    for c in range(kinds):
        for m in range(1, plane):
            own_copy(c, m).start()
    own_in = pltpu.make_async_copy(packed_ref.at[rank], own_s, own_sem.at[0])
    own_in.start()
    channels, length = x_ref.shape
    block = wr_ref.shape[1]
    groups = channels // LANES
    tap_count = taps_ref.shape[1]
    lane = lax.broadcasted_iota(jnp.int32, (LANES, length), 1)

    def local(g, carry):
        rows = pl.ds(pl.multiple_of(g * LANES, LANES), LANES)
        wide = jnp.concatenate(
            [halo_ref[rows, :].astype(jnp.float32), x_ref[rows, :].astype(jnp.float32)], axis=1
        )
        taps = taps_ref[rows, :]
        total = taps[:, tap_count - 1 :] * wide[:, LANES:]
        for tap in range(tap_count - 2, -1, -1):
            total = total + taps[:, tap : tap + 1] * pltpu.roll(wide, tap_count - 1 - tap, 1)[:, LANES:]
        conv = total.astype(jnp.bfloat16)
        per = LANES // block
        recur, admit = [], []
        for b in range(per):
            part = conv[b * block : (b + 1) * block]
            recur.append(jnp.dot(wr_ref[g * per + b], part, preferred_element_type=jnp.float32))
            admit.append(jnp.dot(wa_ref[g * per + b], part, preferred_element_type=jnp.float32))
        recur = jax.nn.sigmoid(jnp.concatenate(recur, axis=0))
        admit = jax.nn.sigmoid(jnp.concatenate(admit, axis=0))
        log_decay = recur * rate_ref[rows, :] + extra_ref[rows, :]
        a = jnp.exp(log_decay)
        b = jnp.sqrt(neg_expm1(2.0 * log_decay)) * admit * conv.astype(jnp.float32)
        shift = 1
        while shift < length:
            seen = lane >= shift
            b = b + a * jnp.where(seen, pltpu.roll(b, shift, 1), 0.0)
            a = a * jnp.where(seen, pltpu.roll(a, shift, 1), 1.0)
            shift *= 2
        state_s[rows, :] = b
        run_s[rows, :] = a
        ends_s[pl.ds(g, 1), :] = a[:, length - LANES :].T[LANES - 1 :]
        ends_s[pl.ds(groups + g, 1), :] = b[:, length - LANES :].T[LANES - 1 :]
        return carry

    lax.fori_loop(0, groups, local, 0)

    own_in.wait()
    own_out = pltpu.make_async_copy(own_s, wide_ref.at[:, :, columns(me)], own_sem.at[1])
    own_out.start()
    z_pass(0)
    z_start(1)
    def copy_to(k):
        return pltpu.make_async_remote_copy(
            src_ref=ends_s,
            dst_ref=all_s.at[k - 1],
            send_sem=send_sem.at[k - 1],
            recv_sem=recv_sem.at[k - 1],
            device_id={"sp": lax.rem(me + k, n)},
            device_id_type=MESH,
        )

    def send(k, carry):
        copy_to(k).start()
        return carry

    lax.fori_loop(1, n, send, 0)

    def finish(k, carry):
        copy_to(k).wait()
        return carry

    lax.fori_loop(1, n, finish, 0)

    def fold(i, before):
        k = n - 1 - i
        part = all_s[k - 1]
        new = part[:groups] * before + part[groups:]
        return jnp.where(k <= me, new, before)

    in_s[...] = lax.fori_loop(0, n - 1, fold, jnp.zeros((groups, LANES), jnp.float32))

    def close(g, carry):
        rows = pl.ds(pl.multiple_of(g * LANES, LANES), LANES)
        entering = jnp.broadcast_to(in_s[pl.ds(g, 1), :], (LANES, LANES)).T
        entering = jnp.concatenate([entering] * (length // LANES), axis=1)
        states = state_s[rows, :] + run_s[rows, :] * entering
        v = bg_ref[rows, :].astype(jnp.float32)
        act = 0.5 * v * (1.0 + jnp.tanh(0.7978845608028654 * (v + 0.044715 * v * v * v)))
        mix_s[:, rows] = (states * act).T.astype(jnp.bfloat16)
        return carry

    lax.fori_loop(0, groups, close, 0)

    pieces, row_count, cut = part_s.shape

    def swap(i):
        return remote(
            part_s.at[i], part_r.at[i], bs_sem.at[i], br_sem.at[i], {"tp": 1 - core}
        )

    for i in range(pieces):
        part_s[i] = jnp.dot(
            mix_s[...], ow_ref[:, i * cut : (i + 1) * cut], preferred_element_type=jnp.float32
        ).astype(jnp.bfloat16)
        if i:
            swap(i - 1).start()
    z_pass(1)
    z_start(2)
    swap(pieces - 1).start()
    square = jnp.zeros((row_count, 1), jnp.float32)
    for i in range(pieces):
        swap(i).wait()
        cols = slice(i * cut, (i + 1) * cut)
        branch = part_s[i].astype(jnp.float32) + part_r[i].astype(jnp.float32)
        middle = (res_ref[:, cols].astype(jnp.float32) + branch).astype(jnp.bfloat16)
        mid_ref[:, cols] = middle
        middle = middle.astype(jnp.float32)
        square = square + jnp.sum(middle * middle, axis=1, keepdims=True)
    scale = lax.rsqrt(square * (1.0 / (pieces * cut)) + 1e-06)
    for i in range(pieces):
        cols = slice(i * cut, (i + 1) * cut)
        middle = mid_ref[:, cols].astype(jnp.float32)
        nrm_s[:, cols] = (middle * scale * gain_ref[:, cols].astype(jnp.float32)).astype(jnp.bfloat16)
    half = row_count // 2
    mine = pl.ds(pl.multiple_of(core * half, half), half)
    other = pl.ds(pl.multiple_of((1 - core) * half, half), half)

    def tok_copy(k):
        to = lax.rem(rank + k, split)
        return remote(
            nrm_s.at[mine, :], tok_ref.at[rank, mine, :],
            ts_sem.at[k - 1], tr_sem.at[k - 1], {"sp": to * plane + spot},
        )

    def tok_landed(k):
        source = lax.rem(rank - k + split, split)
        return remote(
            nrm_s.at[mine, :], tok_ref.at[source, mine, :],
            ts_sem.at[k - 1], tr_sem.at[k - 1], {"sp": source * plane + spot},
        )

    def tok_pass(k, rows):
        source = lax.rem(rank - k + split, split)
        window = tok_ref.at[source, rows, :]
        return remote(window, window, cs_sem.at[k - 1], cr_sem.at[k - 1], {"tp": 1 - core})

    for k in range(1, split):
        tok_copy(k).start()
    own_tok = pltpu.make_async_copy(nrm_s, tok_ref.at[rank], own_sem.at[2])
    own_tok.start()
    z_pass(2)
    for k in range(1, split):
        tok_landed(k).wait_recv()
        tok_pass(k, mine).start()
    for k in range(1, split):
        tok_copy(k).wait_send()
        tok_pass(k, mine).wait_send()
        tok_pass(k, other).wait_recv()
    own_tok.wait()
    own_out.wait()
    for c in range(kinds):
        for m in range(1, plane):
            own_copy(c, m).wait_send()
            own_landed(c, m).wait_recv()
        for k in range(1, split):
            z_copy(c, k).wait_send()
            for m in range(1, plane):
                pass_copy(c, k, m).wait_send()
                pass_landed(c, k, m).wait_recv()


def layer_front(n, split, x, halo, bg, extra, taps, rate, wr, wa, ow, res, gain, packed):
    channels, length = x.shape
    groups = channels // LANES
    rows, width = res.shape
    kinds, span, depth = packed.shape[1:]
    plane = n // split
    cut = 512
    pieces = width // cut
    vmem = pl.BlockSpec(memory_space=pltpu.VMEM)
    hbm = pl.BlockSpec(memory_space=pl.ANY)
    dma = pltpu.SemaphoreType.DMA
    bf16, f32 = jnp.bfloat16, jnp.float32
    return pl.pallas_call(
        functools.partial(layer_kernel, n, split),
        out_shape=(
            jax.ShapeDtypeStruct((kinds, span, n * depth), bf16),
            jax.ShapeDtypeStruct((split, rows, width), bf16),
            jax.ShapeDtypeStruct((rows, width), bf16),
        ),
        in_specs=[vmem] * 11 + [hbm],
        out_specs=(hbm, hbm, vmem),
        scratch_shapes=[
            pltpu.VMEM((channels, length), f32),
            pltpu.VMEM((channels, length), f32),
            pltpu.VMEM((2 * groups, LANES), f32),
            pltpu.VMEM((n - 1, 2 * groups, LANES), f32),
            pltpu.VMEM((groups, LANES), f32),
            pltpu.VMEM((length, channels), bf16),
            pltpu.VMEM((pieces, rows, cut), bf16),
            pltpu.VMEM((pieces, rows, cut), bf16),
            pltpu.VMEM((rows, width), bf16),
            pltpu.VMEM((kinds, span, depth), bf16),
            dma((n - 1,)),
            dma((n - 1,)),
            dma((kinds, split - 1)),
            dma((kinds, split - 1)),
            dma((kinds, plane - 1)),
            dma((kinds, plane - 1)),
            dma((kinds, split - 1, plane - 1)),
            dma((kinds, split - 1, plane - 1)),
            dma((split - 1,)),
            dma((split - 1,)),
            dma((pieces,)),
            dma((pieces,)),
            dma((split - 1,)),
            dma((split - 1,)),
            dma((3,)),
        ],
        compiler_params=pltpu.CompilerParams(
            collective_id=1, has_side_effects=True, vmem_limit_bytes=40 << 20
        ),
        name="layer_front",
    )(x, halo, bg, extra, taps, rate, wr, wa, ow, res, gain, packed)


def close_kernel(
    n, split, part_ref, mid_ref, out_ref,
    tp_s, red_s, z_s, half_s, half_r,
    as_sem, ar_sem, zs_sem, zr_sem, hs_sem, hr_sem,
):
    me = lax.axis_index("sp")
    core = lax.axis_index("tp")
    plane = n // split
    rank, spot = me // plane, lax.rem(me, plane)
    barrier = pltpu.get_barrier_semaphore()
    for k in range(1, split):
        pl.semaphore_signal(
            barrier, inc=1,
            device_id={"sp": lax.rem(rank + k, split) * plane + spot}, device_id_type=MESH,
        )
    pl.semaphore_signal(barrier, inc=1, device_id={"tp": 1 - core}, device_id_type=MESH)
    pl.semaphore_wait(barrier, split)
    half = part_ref.shape[1] // 2
    mine = pl.ds(pl.multiple_of(core * half, half), half)
    other = pl.ds(pl.multiple_of((1 - core) * half, half), half)

    def to_rank(k):
        return lax.rem(rank + k, split)

    def tp_copy(k):
        return pltpu.make_async_remote_copy(
            src_ref=part_ref.at[to_rank(k), other, :], dst_ref=tp_s.at[k],
            send_sem=as_sem.at[k], recv_sem=ar_sem.at[k],
            device_id={"tp": 1 - core}, device_id_type=MESH,
        )

    def z_copy(k):
        return pltpu.make_async_remote_copy(
            src_ref=red_s.at[k - 1], dst_ref=z_s.at[k - 1],
            send_sem=zs_sem.at[k - 1], recv_sem=zr_sem.at[k - 1],
            device_id={"sp": to_rank(k) * plane + spot}, device_id_type=MESH,
        )

    order = list(range(1, split)) + [0]
    for k in order:
        tp_copy(k).start()
    for k in order[:-1]:
        tp_copy(k).wait()
        mixed = part_ref[to_rank(k), mine, :].astype(jnp.float32) + tp_s[k].astype(jnp.float32)
        red_s[k - 1] = mixed.astype(jnp.bfloat16)
        if k > 1:
            z_copy(k - 1).start()
    tp_copy(0).wait()
    z_copy(split - 1).start()
    total = part_ref[rank, mine, :].astype(jnp.float32) + tp_s[0].astype(jnp.float32)
    for k in range(1, split):
        z_copy(k).wait()
        total = total + z_s[k - 1].astype(jnp.float32)
    done = (mid_ref[mine, :].astype(jnp.float32) + total).astype(jnp.bfloat16)
    half_s[...] = done
    out_ref[mine, :] = done
    last = pltpu.make_async_remote_copy(
        src_ref=half_s, dst_ref=half_r, send_sem=hs_sem, recv_sem=hr_sem,
        device_id={"tp": 1 - core}, device_id_type=MESH,
    )
    last.start()
    last.wait()
    out_ref[other, :] = half_r[...]


def layer_close(n, split, part, middle):
    rows, width = middle.shape
    half = rows // 2
    vmem = pl.BlockSpec(memory_space=pltpu.VMEM)
    dma = pltpu.SemaphoreType.DMA
    bf16 = jnp.bfloat16
    return pl.pallas_call(
        functools.partial(close_kernel, n, split),
        out_shape=jax.ShapeDtypeStruct((rows, width), bf16),
        in_specs=[vmem] * 2,
        out_specs=vmem,
        scratch_shapes=[
            pltpu.VMEM((split, half, width), bf16),
            pltpu.VMEM((split - 1, half, width), bf16),
            pltpu.VMEM((split - 1, half, width), bf16),
            pltpu.VMEM((half, width), bf16),
            pltpu.VMEM((half, width), bf16),
            dma((split,)),
            dma((split,)),
            dma((split - 1,)),
            dma((split - 1,)),
            dma,
            dma,
        ],
        compiler_params=pltpu.CompilerParams(
            collective_id=2, has_side_effects=True, vmem_limit_bytes=24 << 20
        ),
        name="layer_close",
    )(part, middle)


def on_device(
    residual_in,
    mixer_input,
    branch_gate,
    conv_taps,
    recur_weight,
    admit_weight,
    decay_param,
    decay_extra,
    out_weight,
    norm_gain,
    gate_weight,
    up_weight,
    down_weight,
):
    n = lax.axis_size("sp")
    length = mixer_input.shape[1]
    halo = lax.ppermute(
        mixer_input[:, length - LANES :], "sp", [(i, i + 1) for i in range(n - 1)]
    )
    rate = -8.0 * jax.nn.softplus(-decay_param)[:, None]
    width, share_ff = residual_in.shape[1], gate_weight.shape[1]
    split = 4
    if (
        lax.axis_size("tp") == 2
        and n % split == 0
        and n > split
        and gate_weight.shape[0] % LANES == 0
        and share_ff % (16 * split) == 0
        and width % 512 == 0
    ):
        span = share_ff // split
        packed = jnp.stack(
            [
                w.reshape(w.shape[0], split, span).transpose(1, 2, 0)
                for w in (gate_weight, up_weight, down_weight)
            ],
            axis=1,
        )
        wide, tokens, middle = layer_front(
            n,
            split,
            mixer_input,
            halo,
            branch_gate,
            decay_extra,
            conv_taps.astype(jnp.float32),
            rate,
            recur_weight.transpose(0, 2, 1),
            admit_weight.transpose(0, 2, 1),
            out_weight,
            residual_in,
            norm_gain.reshape(1, width),
            packed,
        )
        tokens = tokens.reshape(-1, width)
        across = (((1,), (1,)), ((), ()))
        gate_pre = lax.dot_general(tokens, wide[0], across, preferred_element_type=jnp.float32)
        up_pre = lax.dot_general(tokens, wide[1], across, preferred_element_type=jnp.float32)
        hidden = (jax.nn.silu(gate_pre) * up_pre).astype(jnp.bfloat16)
        part = jnp.dot(hidden, wide[2], preferred_element_type=jnp.float32).astype(jnp.bfloat16)
        return layer_close(n, split, part.reshape(split, -1, width), middle)
    mixed_out = mixer(
        n,
        mixer_input,
        halo,
        branch_gate,
        decay_extra,
        conv_taps.astype(jnp.float32),
        rate,
        recur_weight.transpose(0, 2, 1),
        admit_weight.transpose(0, 2, 1),
    )
    row_count = residual_in.shape[0]
    partial_value = lax.dot_general(
        mixed_out, out_weight, (((0,), (0,)), ((), ())), preferred_element_type=jnp.float32
    )
    branch = lax.psum(partial_value.astype(jnp.bfloat16), "tp").astype(jnp.float32)
    middle = (residual_in.astype(jnp.float32) + branch).astype(jnp.bfloat16)
    middle_wide = middle.astype(jnp.float32)
    row_scale = lax.rsqrt(jnp.mean(middle_wide * middle_wide, axis=1, keepdims=True) + 1e-06)
    normed = (middle_wide * row_scale * norm_gain.astype(jnp.float32)).astype(jnp.bfloat16)
    gate_pre = jnp.dot(
        normed,
        lax.all_gather(gate_weight, "sp", axis=0, tiled=True),
        preferred_element_type=jnp.float32,
    )
    up_pre = jnp.dot(
        normed,
        lax.all_gather(up_weight, "sp", axis=0, tiled=True),
        preferred_element_type=jnp.float32,
    )
    down_whole = lax.all_gather(down_weight, "sp", axis=0, tiled=True)
    hidden = (jax.nn.silu(gate_pre) * up_pre).astype(jnp.bfloat16)
    share = row_count // lax.axis_size("tp")
    channel_out = lax.psum_scatter(
        lax.dot_general(
            hidden, down_whole, (((1,), (1,)), ((), ())), preferred_element_type=jnp.float32
        ).astype(jnp.bfloat16),
        "tp",
        scatter_dimension=0,
        tiled=True,
    ).astype(jnp.float32)
    first_row = lax.axis_index("tp") * share
    own_rows = lax.dynamic_slice_in_dim(middle, first_row, share, 0)
    layer_rows = (own_rows.astype(jnp.float32) + channel_out).astype(jnp.bfloat16)
    return lax.all_gather(layer_rows, "tp", axis=0, tiled=True)


def solution(mesh):
    placed = (
        P("sp", None),
        P("tp", "sp"),
        P("tp", "sp"),
        P("tp", None),
        P("tp", None, None),
        P("tp", None, None),
        P("tp"),
        P("tp", "sp"),
        P("tp", None),
        P(),
        P("sp", "tp"),
        P("sp", "tp"),
        P("sp", "tp"),
    )
    return jax.shard_map(
        on_device, mesh=mesh, in_specs=placed, out_specs=P("sp", None), check_vma=False
    )
```

```python
import functools

import jax
import jax.numpy as jnp
from jax import lax
from jax.experimental import pallas as pl
from jax.experimental.pallas import tpu as pltpu
from jax.sharding import PartitionSpec as P

MESH = pl.DeviceIdType.MESH
LANES = 128


def neg_expm1(v):
    series = jnp.full_like(v, 1.0)
    for k in range(9, 1, -1):
        series = 1.0 + series * v * (1.0 / k)
    return jnp.where(v > -0.5, -v * series, 1.0 - jnp.exp(v))


def mixer_kernel(
    n,
    x_ref,
    halo_ref,
    bg_ref,
    extra_ref,
    taps_ref,
    rate_ref,
    wr_ref,
    wa_ref,
    out_ref,
    state_s,
    run_s,
    ends_s,
    all_s,
    in_s,
    send_sem,
    recv_sem,
):
    me = lax.axis_index("sp")
    barrier = pltpu.get_barrier_semaphore()

    def greet(k, carry):
        pl.semaphore_signal(
            barrier, inc=1, device_id={"sp": lax.rem(me + k, n)}, device_id_type=MESH
        )
        return carry

    lax.fori_loop(1, n, greet, 0)
    channels, length = x_ref.shape
    block = wr_ref.shape[1]
    groups = channels // LANES
    tap_count = taps_ref.shape[1]
    lane = lax.broadcasted_iota(jnp.int32, (LANES, length), 1)

    def local(g, carry):
        rows = pl.ds(pl.multiple_of(g * LANES, LANES), LANES)
        wide = jnp.concatenate(
            [halo_ref[rows, :].astype(jnp.float32), x_ref[rows, :].astype(jnp.float32)], axis=1
        )
        taps = taps_ref[rows, :]
        total = taps[:, tap_count - 1 :] * wide[:, LANES:]
        for tap in range(tap_count - 2, -1, -1):
            total = total + taps[:, tap : tap + 1] * pltpu.roll(wide, tap_count - 1 - tap, 1)[:, LANES:]
        conv = total.astype(jnp.bfloat16)
        per = LANES // block
        recur, admit = [], []
        for b in range(per):
            part = conv[b * block : (b + 1) * block]
            recur.append(jnp.dot(wr_ref[g * per + b], part, preferred_element_type=jnp.float32))
            admit.append(jnp.dot(wa_ref[g * per + b], part, preferred_element_type=jnp.float32))
        recur = jax.nn.sigmoid(jnp.concatenate(recur, axis=0))
        admit = jax.nn.sigmoid(jnp.concatenate(admit, axis=0))
        log_decay = recur * rate_ref[rows, :] + extra_ref[rows, :]
        a = jnp.exp(log_decay)
        b = jnp.sqrt(neg_expm1(2.0 * log_decay)) * admit * conv.astype(jnp.float32)
        shift = 1
        while shift < length:
            seen = lane >= shift
            b = b + a * jnp.where(seen, pltpu.roll(b, shift, 1), 0.0)
            a = a * jnp.where(seen, pltpu.roll(a, shift, 1), 1.0)
            shift *= 2
        state_s[rows, :] = b
        run_s[rows, :] = a
        ends_s[pl.ds(g, 1), :] = a[:, length - LANES :].T[LANES - 1 :]
        ends_s[pl.ds(groups + g, 1), :] = b[:, length - LANES :].T[LANES - 1 :]
        return carry

    lax.fori_loop(0, groups, local, 0)
    pl.semaphore_wait(barrier, n - 1)

    def copy_to(k):
        return pltpu.make_async_remote_copy(
            src_ref=ends_s,
            dst_ref=all_s.at[k - 1],
            send_sem=send_sem.at[k - 1],
            recv_sem=recv_sem.at[k - 1],
            device_id={"sp": lax.rem(me + k, n)},
            device_id_type=MESH,
        )

    def send(k, carry):
        copy_to(k).start()
        return carry

    lax.fori_loop(1, n, send, 0)

    def finish(k, carry):
        copy_to(k).wait()
        return carry

    lax.fori_loop(1, n, finish, 0)

    def fold(i, before):
        k = n - 1 - i
        part = all_s[k - 1]
        new = part[:groups] * before + part[groups:]
        return jnp.where(k <= me, new, before)

    in_s[...] = lax.fori_loop(0, n - 1, fold, jnp.zeros((groups, LANES), jnp.float32))

    def close(g, carry):
        rows = pl.ds(pl.multiple_of(g * LANES, LANES), LANES)
        entering = jnp.broadcast_to(in_s[pl.ds(g, 1), :], (LANES, LANES)).T
        entering = jnp.concatenate([entering] * (length // LANES), axis=1)
        states = state_s[rows, :] + run_s[rows, :] * entering
        v = bg_ref[rows, :].astype(jnp.float32)
        act = 0.5 * v * (1.0 + jnp.tanh(0.7978845608028654 * (v + 0.044715 * v * v * v)))
        out_ref[rows, :] = (states * act).astype(jnp.bfloat16)
        return carry

    lax.fori_loop(0, groups, close, 0)


def mixer(n, x, halo, bg, extra, taps, rate, wr, wa):
    channels, length = x.shape
    groups = channels // LANES
    vmem = pl.BlockSpec(memory_space=pltpu.VMEM)
    return pl.pallas_call(
        functools.partial(mixer_kernel, n),
        out_shape=jax.ShapeDtypeStruct((channels, length), jnp.bfloat16),
        in_specs=[vmem] * 8,
        out_specs=vmem,
        scratch_shapes=[
            pltpu.VMEM((channels, length), jnp.float32),
            pltpu.VMEM((channels, length), jnp.float32),
            pltpu.VMEM((2 * groups, LANES), jnp.float32),
            pltpu.VMEM((n - 1, 2 * groups, LANES), jnp.float32),
            pltpu.VMEM((groups, LANES), jnp.float32),
            pltpu.SemaphoreType.DMA((n - 1,)),
            pltpu.SemaphoreType.DMA((n - 1,)),
        ],
        compiler_params=pltpu.CompilerParams(
            collective_id=0, has_side_effects=True, vmem_limit_bytes=24 << 20
        ),
        cost_estimate=pl.CostEstimate(
            flops=200 * channels * length, bytes_accessed=12 * channels * length, transcendentals=0
        ),
        name="mixer",
    )(x, halo, bg, extra, taps, rate, wr, wa)


def layer_kernel(
    n,
    split,
    x_ref,
    bg_ref,
    extra_ref,
    taps_ref,
    rate_ref,
    wr_ref,
    wa_ref,
    ow_ref,
    res_ref,
    gain_ref,
    packed_ref,
    wide_ref,
    tok_ref,
    mid_ref,
    halo_ref,
    state_s,
    run_s,
    ends_s,
    all_s,
    in_s,
    mix_s,
    part_s,
    part_r,
    nrm_s,
    own_s,
    send_sem,
    recv_sem,
    zs_sem,
    zr_sem,
    ps_sem,
    pr_sem,
    fs_sem,
    fr_sem,
    ts_sem,
    tr_sem,
    bs_sem,
    br_sem,
    cs_sem,
    cr_sem,
    own_sem,
    hs_sem,
    hr_sem,
    rs_sem,
    rr_sem,
):
    me = lax.axis_index("sp")
    core = lax.axis_index("tp")
    plane = n // split
    rank, spot = me // plane, lax.rem(me, plane)
    barrier = pltpu.get_barrier_semaphore()

    def greet(k, carry):
        pl.semaphore_signal(
            barrier, inc=1, device_id={"sp": lax.rem(me + k, n)}, device_id_type=MESH
        )
        return carry

    lax.fori_loop(1, n, greet, 0)
    pl.semaphore_signal(barrier, inc=1, device_id={"tp": 1 - core}, device_id_type=MESH)
    pl.semaphore_wait(barrier, n)

    depth = packed_ref.shape[3]
    span = packed_ref.shape[2]
    kinds = packed_ref.shape[1]

    def columns(source):
        return pl.ds(pl.multiple_of(source * depth, depth), depth)

    def remote(src, dst, ssem, rsem, where):
        return pltpu.make_async_remote_copy(
            src_ref=src, dst_ref=dst, send_sem=ssem, recv_sem=rsem,
            device_id=where, device_id_type=MESH,
        )

    def z_copy(c, k):
        to = lax.rem(rank + k, split)
        return remote(
            packed_ref.at[to, c], wide_ref.at[c, :, columns(me)],
            zs_sem.at[c, k - 1], zr_sem.at[c, k - 1], {"sp": to * plane + spot},
        )

    def z_landed(c, k):
        source = lax.rem(rank - k + split, split) * plane + spot
        return remote(
            packed_ref.at[rank, c], wide_ref.at[c, :, columns(source)],
            zs_sem.at[c, k - 1], zr_sem.at[c, k - 1], {"sp": source},
        )

    def beside(m):
        return spot + 1 - 2 * lax.rem(spot, 2) if m == 1 else spot + 2 - 4 * (spot // 2)

    def own_copy(c, m):
        return remote(
            packed_ref.at[rank, c], wide_ref.at[c, :, columns(me)],
            ps_sem.at[c, m - 1], pr_sem.at[c, m - 1],
            {"sp": rank * plane + beside(m)},
        )

    def own_landed(c, m):
        source = rank * plane + beside(m)
        return remote(
            packed_ref.at[rank, c], wide_ref.at[c, :, columns(source)],
            ps_sem.at[c, m - 1], pr_sem.at[c, m - 1], {"sp": source},
        )

    def pass_copy(c, k, m):
        source = lax.rem(rank - k + split, split) * plane + spot
        window = wide_ref.at[c, :, columns(source)]
        return remote(
            window, window, fs_sem.at[c, k - 1, m - 1], fr_sem.at[c, k - 1, m - 1],
            {"sp": rank * plane + beside(m)},
        )

    def pass_landed(c, k, m):
        behind = beside(m)
        source = lax.rem(rank - k + split, split) * plane + behind
        window = wide_ref.at[c, :, columns(source)]
        return remote(
            window, window, fs_sem.at[c, k - 1, m - 1], fr_sem.at[c, k - 1, m - 1],
            {"sp": rank * plane + behind},
        )

    def relay_window(c, k, m, where):
        source = lax.rem(rank - k + split, split) * plane + where
        return wide_ref.at[c, pl.ds((m - 1) * (span // 2), span // 2), columns(source)]

    def relay_copy(c, k, m):
        window = relay_window(c, k, m, beside(m))
        return remote(
            window, window, rs_sem.at[c, k, m - 1], rr_sem.at[c, k, m - 1],
            {"sp": rank * plane + beside(3 - m)},
        )

    def relay_landed(c, k, m):
        window = relay_window(c, k, m, 3 - spot)
        return remote(
            window, window, rs_sem.at[c, k, m - 1], rr_sem.at[c, k, m - 1],
            {"sp": rank * plane + beside(3 - m)},
        )

    def relay(c, k):
        for m in (1, 2):
            landed = pass_landed(c, k, m) if k else own_landed(c, m)
            landed.wait_recv()
            relay_copy(c, k, m).start()

    def z_start(c):
        for k in range(1, split):
            z_copy(c, k).start()

    def z_pass(c):
        for k in range(1, split):
            z_landed(c, k).wait_recv()
            for m in (1, 2):
                pass_copy(c, k, m).start()

    halo_copy = remote(
        x_ref.at[:, pl.ds(x_ref.shape[1] - LANES, LANES)], halo_ref, hs_sem, hr_sem,
        {"sp": lax.rem(me + 1, n)},
    )
    halo_copy.start()
    z_start(0)
    for c in range(kinds):
        for m in (1, 2):
            own_copy(c, m).start()
    own_in = pltpu.make_async_copy(packed_ref.at[rank], own_s, own_sem.at[0])
    own_in.start()
    halo_copy.wait()
    inside = jnp.where(me > 0, 1.0, 0.0)
    channels, length = x_ref.shape
    block = wr_ref.shape[1]
    groups = channels // LANES
    tap_count = taps_ref.shape[1]
    lane = lax.broadcasted_iota(jnp.int32, (LANES, length), 1)

    def local(g, carry):
        rows = pl.ds(pl.multiple_of(g * LANES, LANES), LANES)
        wide = jnp.concatenate(
            [halo_ref[rows, :].astype(jnp.float32) * inside, x_ref[rows, :].astype(jnp.float32)], axis=1
        )
        taps = taps_ref[rows, :]
        total = taps[:, tap_count - 1 :] * wide[:, LANES:]
        for tap in range(tap_count - 2, -1, -1):
            total = total + taps[:, tap : tap + 1] * pltpu.roll(wide, tap_count - 1 - tap, 1)[:, LANES:]
        conv = total.astype(jnp.bfloat16)
        per = LANES // block
        recur, admit = [], []
        for b in range(per):
            part = conv[b * block : (b + 1) * block]
            recur.append(jnp.dot(wr_ref[g * per + b], part, preferred_element_type=jnp.float32))
            admit.append(jnp.dot(wa_ref[g * per + b], part, preferred_element_type=jnp.float32))
        recur = jax.nn.sigmoid(jnp.concatenate(recur, axis=0))
        admit = jax.nn.sigmoid(jnp.concatenate(admit, axis=0))
        log_decay = recur * rate_ref[rows, :] + extra_ref[rows, :]
        a = jnp.exp(log_decay)
        b = jnp.sqrt(neg_expm1(2.0 * log_decay)) * admit * conv.astype(jnp.float32)
        shift = 1
        while shift < length:
            seen = lane >= shift
            b = b + a * jnp.where(seen, pltpu.roll(b, shift, 1), 0.0)
            a = a * jnp.where(seen, pltpu.roll(a, shift, 1), 1.0)
            shift *= 2
        state_s[rows, :] = b
        run_s[rows, :] = a
        ends_s[pl.ds(g, 1), :] = a[:, length - LANES :].T[LANES - 1 :]
        ends_s[pl.ds(groups + g, 1), :] = b[:, length - LANES :].T[LANES - 1 :]
        return carry

    lax.fori_loop(0, groups, local, 0)

    own_in.wait()
    own_out = pltpu.make_async_copy(own_s, wide_ref.at[:, :, columns(me)], own_sem.at[1])
    own_out.start()
    relay(0, 0)
    z_pass(0)
    z_start(1)
    def copy_to(k):
        return pltpu.make_async_remote_copy(
            src_ref=ends_s,
            dst_ref=all_s.at[k - 1],
            send_sem=send_sem.at[k - 1],
            recv_sem=recv_sem.at[k - 1],
            device_id={"sp": lax.rem(me + k, n)},
            device_id_type=MESH,
        )

    def send(k, carry):
        copy_to(k).start()
        return carry

    lax.fori_loop(1, n, send, 0)

    def finish(k, carry):
        copy_to(k).wait()
        return carry

    lax.fori_loop(1, n, finish, 0)

    def fold(i, before):
        k = n - 1 - i
        part = all_s[k - 1]
        new = part[:groups] * before + part[groups:]
        return jnp.where(k <= me, new, before)

    in_s[...] = lax.fori_loop(0, n - 1, fold, jnp.zeros((groups, LANES), jnp.float32))

    def close(g, carry):
        rows = pl.ds(pl.multiple_of(g * LANES, LANES), LANES)
        entering = jnp.broadcast_to(in_s[pl.ds(g, 1), :], (LANES, LANES)).T
        entering = jnp.concatenate([entering] * (length // LANES), axis=1)
        states = state_s[rows, :] + run_s[rows, :] * entering
        v = bg_ref[rows, :].astype(jnp.float32)
        act = 0.5 * v * (1.0 + jnp.tanh(0.7978845608028654 * (v + 0.044715 * v * v * v)))
        mix_s[:, rows] = (states * act).T.astype(jnp.bfloat16)
        return carry

    lax.fori_loop(0, groups, close, 0)

    pieces, row_count, cut = part_s.shape

    def swap(i):
        return remote(
            part_s.at[i], part_r.at[i], bs_sem.at[i], br_sem.at[i], {"tp": 1 - core}
        )

    for i in range(pieces):
        part_s[i] = jnp.dot(
            mix_s[...], ow_ref[:, i * cut : (i + 1) * cut], preferred_element_type=jnp.float32
        ).astype(jnp.bfloat16)
        if i:
            swap(i - 1).start()
    z_pass(1)
    z_start(2)
    swap(pieces - 1).start()
    square = jnp.zeros((row_count, 1), jnp.float32)
    for i in range(pieces):
        swap(i).wait()
        cols = slice(i * cut, (i + 1) * cut)
        branch = part_s[i].astype(jnp.float32) + part_r[i].astype(jnp.float32)
        middle = (res_ref[:, cols].astype(jnp.float32) + branch).astype(jnp.bfloat16)
        mid_ref[:, cols] = middle
        middle = middle.astype(jnp.float32)
        square = square + jnp.sum(middle * middle, axis=1, keepdims=True)
    scale = lax.rsqrt(square * (1.0 / (pieces * cut)) + 1e-06)
    for i in range(pieces):
        cols = slice(i * cut, (i + 1) * cut)
        middle = mid_ref[:, cols].astype(jnp.float32)
        nrm_s[:, cols] = (middle * scale * gain_ref[:, cols].astype(jnp.float32)).astype(jnp.bfloat16)
    half = row_count // 2
    mine = pl.ds(pl.multiple_of(core * half, half), half)
    other = pl.ds(pl.multiple_of((1 - core) * half, half), half)

    def tok_copy(k):
        to = lax.rem(rank + k, split)
        return remote(
            nrm_s.at[mine, :], tok_ref.at[rank, mine, :],
            ts_sem.at[k - 1], tr_sem.at[k - 1], {"sp": to * plane + spot},
        )

    def tok_landed(k):
        source = lax.rem(rank - k + split, split)
        return remote(
            nrm_s.at[mine, :], tok_ref.at[source, mine, :],
            ts_sem.at[k - 1], tr_sem.at[k - 1], {"sp": source * plane + spot},
        )

    def tok_pass(k, rows):
        source = lax.rem(rank - k + split, split)
        window = tok_ref.at[source, rows, :]
        return remote(window, window, cs_sem.at[k - 1], cr_sem.at[k - 1], {"tp": 1 - core})

    for k in range(1, split):
        tok_copy(k).start()
    own_tok = pltpu.make_async_copy(nrm_s, tok_ref.at[rank], own_sem.at[2])
    own_tok.start()
    relay(1, 0)
    relay(2, 0)
    for k in range(1, split):
        relay(0, k)
    z_pass(2)
    for k in range(1, split):
        relay(1, k)
    for k in range(1, split):
        tok_landed(k).wait_recv()
        tok_pass(k, mine).start()
    for k in range(1, split):
        tok_copy(k).wait_send()
        tok_pass(k, mine).wait_send()
        tok_pass(k, other).wait_recv()
    own_tok.wait()
    own_out.wait()
    for k in range(1, split):
        relay(2, k)
    for c in range(kinds):
        for m in (1, 2):
            own_copy(c, m).wait_send()
        for k in range(split):
            for m in (1, 2):
                if k:
                    pass_copy(c, k, m).wait_send()
                relay_copy(c, k, m).wait_send()
                relay_landed(c, k, m).wait_recv()
            if k:
                z_copy(c, k).wait_send()


def layer_front(n, split, x, bg, extra, taps, rate, wr, wa, ow, res, gain, packed):
    channels, length = x.shape
    groups = channels // LANES
    rows, width = res.shape
    kinds, span, depth = packed.shape[1:]
    plane = n // split
    cut = 512
    pieces = width // cut
    vmem = pl.BlockSpec(memory_space=pltpu.VMEM)
    hbm = pl.BlockSpec(memory_space=pl.ANY)
    dma = pltpu.SemaphoreType.DMA
    bf16, f32 = jnp.bfloat16, jnp.float32
    return pl.pallas_call(
        functools.partial(layer_kernel, n, split),
        out_shape=(
            jax.ShapeDtypeStruct((kinds, span, n * depth), bf16),
            jax.ShapeDtypeStruct((split, rows, width), bf16),
            jax.ShapeDtypeStruct((rows, width), bf16),
        ),
        in_specs=[vmem] * 10 + [hbm],
        out_specs=(hbm, hbm, vmem),
        scratch_shapes=[
            pltpu.VMEM((channels, LANES), bf16),
            pltpu.VMEM((channels, length), f32),
            pltpu.VMEM((channels, length), f32),
            pltpu.VMEM((2 * groups, LANES), f32),
            pltpu.VMEM((n - 1, 2 * groups, LANES), f32),
            pltpu.VMEM((groups, LANES), f32),
            pltpu.VMEM((length, channels), bf16),
            pltpu.VMEM((pieces, rows, cut), bf16),
            pltpu.VMEM((pieces, rows, cut), bf16),
            pltpu.VMEM((rows, width), bf16),
            pltpu.VMEM((kinds, span, depth), bf16),
            dma((n - 1,)),
            dma((n - 1,)),
            dma((kinds, split - 1)),
            dma((kinds, split - 1)),
            dma((kinds, 2)),
            dma((kinds, 2)),
            dma((kinds, split - 1, 2)),
            dma((kinds, split - 1, 2)),
            dma((split - 1,)),
            dma((split - 1,)),
            dma((pieces,)),
            dma((pieces,)),
            dma((split - 1,)),
            dma((split - 1,)),
            dma((3,)),
            dma,
            dma,
            dma((kinds, split, 2)),
            dma((kinds, split, 2)),
        ],
        compiler_params=pltpu.CompilerParams(
            collective_id=1, has_side_effects=True, vmem_limit_bytes=40 << 20
        ),
        name="layer_front",
    )(x, bg, extra, taps, rate, wr, wa, ow, res, gain, packed)


def close_kernel(
    n, split, tok_ref, wide_ref, mid_ref, out_ref,
    part_ref, tok_s, wide_s, tk_sem, wd_sem, tp_s, red_s, z_s, half_s, half_r,
    as_sem, ar_sem, zs_sem, zr_sem, hs_sem, hr_sem,
):
    me = lax.axis_index("sp")
    core = lax.axis_index("tp")
    plane = n // split
    rank, spot = me // plane, lax.rem(me, plane)
    barrier = pltpu.get_barrier_semaphore()
    order = list(range(1, split)) + [0]
    kinds = wide_ref.shape[0]

    def tok_in(k):
        return pltpu.make_async_copy(
            tok_ref.at[lax.rem(rank + k, split)], tok_s.at[k], tk_sem.at[k]
        )

    def wide_in(c):
        return pltpu.make_async_copy(wide_ref.at[c], wide_s.at[c], wd_sem.at[c])

    tok_in(order[0]).start()
    for c in range(kinds):
        wide_in(c).start()
    for k in order[1:]:
        tok_in(k).start()
    for k in range(1, split):
        pl.semaphore_signal(
            barrier, inc=1,
            device_id={"sp": lax.rem(rank + k, split) * plane + spot}, device_id_type=MESH,
        )
    pl.semaphore_signal(barrier, inc=1, device_id={"tp": 1 - core}, device_id_type=MESH)
    def feed(k):
        tok_in(k).wait()
        across = (((1,), (1,)), ((), ()))
        if k == order[0]:
            wide_in(0).wait()
        gate = lax.dot_general(tok_s[k], wide_s[0], across, preferred_element_type=jnp.float32)
        if k == order[0]:
            wide_in(1).wait()
        up = lax.dot_general(tok_s[k], wide_s[1], across, preferred_element_type=jnp.float32)
        hidden = (gate / (1.0 + jnp.exp(-gate)) * up).astype(jnp.bfloat16)
        if k == order[0]:
            wide_in(2).wait()
        part_ref[k] = jnp.dot(
            hidden, wide_s[2], preferred_element_type=jnp.float32
        ).astype(jnp.bfloat16)

    half = mid_ref.shape[0] // 2
    mine = pl.ds(pl.multiple_of(core * half, half), half)
    other = pl.ds(pl.multiple_of((1 - core) * half, half), half)

    def to_rank(k):
        return lax.rem(rank + k, split)

    def tp_copy(k):
        return pltpu.make_async_remote_copy(
            src_ref=part_ref.at[k, other, :], dst_ref=tp_s.at[k],
            send_sem=as_sem.at[k], recv_sem=ar_sem.at[k],
            device_id={"tp": 1 - core}, device_id_type=MESH,
        )

    def z_copy(k):
        return pltpu.make_async_remote_copy(
            src_ref=red_s.at[k - 1], dst_ref=z_s.at[k - 1],
            send_sem=zs_sem.at[k - 1], recv_sem=zr_sem.at[k - 1],
            device_id={"sp": to_rank(k) * plane + spot}, device_id_type=MESH,
        )

    def reduce(k):
        tp_copy(k).wait()
        mixed = part_ref[k, mine, :].astype(jnp.float32) + tp_s[k].astype(jnp.float32)
        red_s[k - 1] = mixed.astype(jnp.bfloat16)

    feed(1)
    pl.semaphore_wait(barrier, split)
    tp_copy(1).start()
    for k in range(2, split):
        feed(k)
        tp_copy(k).start()
        reduce(k - 1)
        z_copy(k - 1).start()
    reduce(split - 1)
    z_copy(split - 1).start()
    feed(0)
    tp_copy(0).start()
    tp_copy(0).wait()
    total = part_ref[0, mine, :].astype(jnp.float32) + tp_s[0].astype(jnp.float32)
    for k in range(1, split):
        z_copy(k).wait()
        total = total + z_s[k - 1].astype(jnp.float32)
    done = (mid_ref[mine, :].astype(jnp.float32) + total).astype(jnp.bfloat16)
    half_s[...] = done
    out_ref[mine, :] = done
    last = pltpu.make_async_remote_copy(
        src_ref=half_s, dst_ref=half_r, send_sem=hs_sem, recv_sem=hr_sem,
        device_id={"tp": 1 - core}, device_id_type=MESH,
    )
    last.start()
    last.wait()
    out_ref[other, :] = half_r[...]


def layer_close(n, split, tokens, wide, middle):
    rows, width = middle.shape
    half = rows // 2
    vmem = pl.BlockSpec(memory_space=pltpu.VMEM)
    dma = pltpu.SemaphoreType.DMA
    bf16 = jnp.bfloat16
    return pl.pallas_call(
        functools.partial(close_kernel, n, split),
        out_shape=jax.ShapeDtypeStruct((rows, width), bf16),
        in_specs=[pl.BlockSpec(memory_space=pl.ANY)] * 2 + [vmem],
        out_specs=vmem,
        scratch_shapes=[
            pltpu.VMEM((split, rows, width), bf16),
            pltpu.VMEM((split, rows, width), bf16),
            pltpu.VMEM(wide.shape, bf16),
            dma((split,)),
            dma((wide.shape[0],)),
            pltpu.VMEM((split, half, width), bf16),
            pltpu.VMEM((split - 1, half, width), bf16),
            pltpu.VMEM((split - 1, half, width), bf16),
            pltpu.VMEM((half, width), bf16),
            pltpu.VMEM((half, width), bf16),
            dma((split,)),
            dma((split,)),
            dma((split - 1,)),
            dma((split - 1,)),
            dma,
            dma,
        ],
        compiler_params=pltpu.CompilerParams(
            collective_id=2, has_side_effects=True, vmem_limit_bytes=48 << 20
        ),
        name="layer_close",
    )(tokens, wide, middle)


def on_device(
    residual_in,
    mixer_input,
    branch_gate,
    conv_taps,
    recur_weight,
    admit_weight,
    decay_param,
    decay_extra,
    out_weight,
    norm_gain,
    gate_weight,
    up_weight,
    down_weight,
):
    n = lax.axis_size("sp")
    length = mixer_input.shape[1]
    halo = lax.ppermute(
        mixer_input[:, length - LANES :], "sp", [(i, i + 1) for i in range(n - 1)]
    )
    rate = -8.0 * jax.nn.softplus(-decay_param)[:, None]
    width, share_ff = residual_in.shape[1], gate_weight.shape[1]
    split = 4
    if (
        lax.axis_size("tp") == 2
        and n == 4 * split
        and gate_weight.shape[0] % LANES == 0
        and share_ff % (32 * split) == 0
        and width % 512 == 0
    ):
        span = share_ff // split
        packed = jnp.stack(
            [
                w.reshape(w.shape[0], split, span).transpose(1, 2, 0)
                for w in (gate_weight, up_weight, down_weight)
            ],
            axis=1,
        )
        wide, tokens, middle = layer_front(
            n,
            split,
            mixer_input,
            branch_gate,
            decay_extra,
            conv_taps.astype(jnp.float32),
            rate,
            recur_weight.transpose(0, 2, 1),
            admit_weight.transpose(0, 2, 1),
            out_weight,
            residual_in,
            norm_gain.reshape(1, width),
            packed,
        )
        return layer_close(n, split, tokens, wide, middle)
    mixed_out = mixer(
        n,
        mixer_input,
        halo,
        branch_gate,
        decay_extra,
        conv_taps.astype(jnp.float32),
        rate,
        recur_weight.transpose(0, 2, 1),
        admit_weight.transpose(0, 2, 1),
    )
    row_count = residual_in.shape[0]
    partial_value = lax.dot_general(
        mixed_out, out_weight, (((0,), (0,)), ((), ())), preferred_element_type=jnp.float32
    )
    branch = lax.psum(partial_value.astype(jnp.bfloat16), "tp").astype(jnp.float32)
    middle = (residual_in.astype(jnp.float32) + branch).astype(jnp.bfloat16)
    middle_wide = middle.astype(jnp.float32)
    row_scale = lax.rsqrt(jnp.mean(middle_wide * middle_wide, axis=1, keepdims=True) + 1e-06)
    normed = (middle_wide * row_scale * norm_gain.astype(jnp.float32)).astype(jnp.bfloat16)
    gate_pre = jnp.dot(
        normed,
        lax.all_gather(gate_weight, "sp", axis=0, tiled=True),
        preferred_element_type=jnp.float32,
    )
    up_pre = jnp.dot(
        normed,
        lax.all_gather(up_weight, "sp", axis=0, tiled=True),
        preferred_element_type=jnp.float32,
    )
    down_whole = lax.all_gather(down_weight, "sp", axis=0, tiled=True)
    hidden = (jax.nn.silu(gate_pre) * up_pre).astype(jnp.bfloat16)
    share = row_count // lax.axis_size("tp")
    channel_out = lax.psum_scatter(
        lax.dot_general(
            hidden, down_whole, (((1,), (1,)), ((), ())), preferred_element_type=jnp.float32
        ).astype(jnp.bfloat16),
        "tp",
        scatter_dimension=0,
        tiled=True,
    ).astype(jnp.float32)
    first_row = lax.axis_index("tp") * share
    own_rows = lax.dynamic_slice_in_dim(middle, first_row, share, 0)
    layer_rows = (own_rows.astype(jnp.float32) + channel_out).astype(jnp.bfloat16)
    return lax.all_gather(layer_rows, "tp", axis=0, tiled=True)


def solution(mesh):
    placed = (
        P("sp", None),
        P("tp", "sp"),
        P("tp", "sp"),
        P("tp", None),
        P("tp", None, None),
        P("tp", None, None),
        P("tp"),
        P("tp", "sp"),
        P("tp", None),
        P(),
        P("sp", "tp"),
        P("sp", "tp"),
        P("sp", "tp"),
    )
    return jax.shard_map(
        on_device, mesh=mesh, in_specs=placed, out_specs=P("sp", None), check_vma=False
    )
```
